32 devices in a mesh: rep: 2 (over x), fs: 8 (over z, y), tp: 2 (over core).
Axes of the slice: x: 2, y: 2, z: 4, core: 2. Of those that a mesh axis runs over, the one named last changes fastest.
Arguments:
- tokens: bfloat16 [6144, 2048], P(('rep', 'fs'), 'tp'), may hold values from -6 to 6
- mixing_norm_gain: float32 [2048], replicated, may hold values from 0.1 to 1.9
- recurrent_input_weight: float32 [2048, 3072], P('fs', 'tp'), may hold values from -0.125 to 0.125
- recurrent_input_scale: float32 [3072], P('tp'), may hold values from 0.5 to 2
- convolution_kernel_taps: float32 [4, 3072], P(None, 'tp'), may hold values from -3 to 3
- recurrence_gate_weight_blocks: bfloat16 [24, 128, 128], P('tp'), may hold values from -0.5 to 0.5
- input_gate_weight_blocks: bfloat16 [24, 128, 128], P('tp'), may hold values from -0.5 to 0.5
- channel_decay_parameter: float32 [3072], P('tp'), may hold values from 3 to 9
- token_extra_log_decay: float32 [6144], P(('rep', 'fs')), may hold values from -0.7 to 0
- mixing_output_weight: float32 [3072, 2048], P('tp', 'fs'), may hold values from -0.109375 to 0.109375
- mixing_output_scale: float32 [2048], P('fs'), may hold values from 0.5 to 2
- feedforward_norm_gain: float32 [2048], replicated, may hold values from 0.1 to 1.9
- feedforward_gate_weight: float32 [2048, 5120], P('fs', 'tp'), may hold values from -0.125 to 0.125
- feedforward_gate_scale: float32 [5120], P('tp'), may hold values from 0.5 to 2
- feedforward_up_weight: float32 [2048, 5120], P('fs', 'tp'), may hold values from -0.125 to 0.125
- feedforward_up_scale: float32 [5120], P('tp'), may hold values from 0.5 to 2
- feedforward_down_weight: float32 [5120, 2048], P('tp', 'fs'), may hold values from -0.078125 to 0.078125
- feedforward_down_scale: float32 [2048], P('fs'), may hold values from 0.5 to 2
Outputs:
- layer_out: bfloat16 [6144, 2048], P(('rep', 'fs'), 'tp')
The draws below stay inside these ranges and needn't reach their ends.
All inputs are finite; a program needn't handle non-finite values.
Results may differ from the reference program's by a relative error of at most 0.02.
Values may be sent and summed in bfloat16 or wider, within the bound.
A program may use at most 128 MiB of HBM per device.

```python
import math
import jax
import jax.numpy as jnp
from jax import lax

MODEL_DIM = 2048
W = 3072
FF = 5120
BLOCK = 128
CONV = 4
SEQUENCE_LENGTH = 384
NB = 24
TOKENS = 6144
N_TP = 2


def draw_token_extra_log_decay(key, part):
    first_key, second_key = jax.random.split(jax.random.fold_in(key, 17))
    chosen = jax.random.randint(first_key, (TOKENS,), 0, 64) == 0
    depth = jax.random.uniform(second_key, (TOKENS,), jnp.float32, 0.22, 0.7)
    return jnp.where(chosen, -depth, 0.0).astype(jnp.float32)


def block_levels(key, dims, pieces, least, high):
    level = 1.0
    for dim, shards_of in pieces:
        draws = jax.random.uniform(jax.random.fold_in(jax.random.fold_in(key, 6), dim), (shards_of,), jnp.float32, least / len(pieces), high / len(pieces))
        level = level * jnp.repeat(jnp.exp(draws), dims[dim] // shards_of).reshape((-1,) + (1,) * (len(dims) - 1 - dim))
    return level


def scatter_about(key, extent, scale, reach, pieces=(), held_as=jnp.bfloat16):
    result = jax.random.normal(key, extent, jnp.float32) * scale
    if len(pieces) > 0:
        result = block_levels(key, extent, pieces, -0.22, 0.18) * result
    return jnp.clip(result, min=-reach, max=reach).astype(held_as)


def setup_inputs(seed: int = 0) -> dict:
    key_of = jax.random.split(jax.random.key(seed), 19)
    return {
        "tokens": scatter_about(key_of[0], (TOKENS, MODEL_DIM), 1.0, 6.0, ((0, 16), (1, 2))),
        "mixing_norm_gain": jnp.clip(1.0 + 0.18 * jax.random.normal(key_of[1], (MODEL_DIM,), jnp.float32), 0.1, 1.9),
        "recurrent_input_weight": scatter_about(key_of[2], (MODEL_DIM, W), MODEL_DIM ** -0.5, 0.125, ((0, 8), (1, 2)), jnp.float32),
        "recurrent_input_scale": jnp.clip(jnp.exp(math.log(2.0) - 1.3862944 * jax.random.uniform(key_of[3], (W,), jnp.float32) ** block_levels(key_of[3], (W,), ((0, 2),), -0.2, 0.2)), 0.5, 2.0),
        "convolution_kernel_taps": scatter_about(key_of[4], (CONV, W), 0.5, 3.0, ((1, 2),), jnp.float32),
        "recurrence_gate_weight_blocks": scatter_about(key_of[5], (NB, BLOCK, BLOCK), BLOCK ** -0.5, 0.5, ((0, 2),)),
        "input_gate_weight_blocks": scatter_about(key_of[6], (NB, BLOCK, BLOCK), BLOCK ** -0.5, 0.5, ((0, 2),)),
        "channel_decay_parameter": jnp.clip(3.0 + 6.0 * jax.random.uniform(key_of[7], (W,), jnp.float32) ** block_levels(key_of[7], (W,), ((0, 2),), -0.2, 0.2), 3.0, 9.0),
        "token_extra_log_decay": draw_token_extra_log_decay(jax.random.fold_in(key_of[18], 71), 0),
        "mixing_output_weight": scatter_about(key_of[9], (W, MODEL_DIM), W ** -0.5, 0.109375, ((0, 2), (1, 8)), jnp.float32),
        "mixing_output_scale": jnp.clip(jnp.exp(math.log(2.0) - 1.3862944 * jax.random.uniform(key_of[10], (MODEL_DIM,), jnp.float32) ** block_levels(key_of[10], (MODEL_DIM,), ((0, 8),), -0.2, 0.2)), 0.5, 2.0),
        "feedforward_norm_gain": jnp.clip(1.0 + 0.18 * jax.random.normal(key_of[11], (MODEL_DIM,), jnp.float32), 0.1, 1.9),
        "feedforward_gate_weight": scatter_about(key_of[12], (MODEL_DIM, FF), MODEL_DIM ** -0.5, 0.125, ((0, 8), (1, 2)), jnp.float32),
        "feedforward_gate_scale": jnp.clip(jnp.exp(math.log(2.0) - 1.3862944 * jax.random.uniform(key_of[13], (FF,), jnp.float32) ** block_levels(key_of[13], (FF,), ((0, 2),), -0.2, 0.2)), 0.5, 2.0),
        "feedforward_up_weight": scatter_about(key_of[14], (MODEL_DIM, FF), MODEL_DIM ** -0.5, 0.125, ((0, 8), (1, 2)), jnp.float32),
        "feedforward_up_scale": jnp.clip(jnp.exp(math.log(2.0) - 1.3862944 * jax.random.uniform(key_of[15], (FF,), jnp.float32) ** block_levels(key_of[15], (FF,), ((0, 2),), -0.2, 0.2)), 0.5, 2.0),
        "feedforward_down_weight": scatter_about(key_of[16], (FF, MODEL_DIM), FF ** -0.5, 0.078125, ((0, 2), (1, 8)), jnp.float32),
        "feedforward_down_scale": jnp.clip(jnp.exp(math.log(2.0) - 1.3862944 * jax.random.uniform(key_of[17], (MODEL_DIM,), jnp.float32) ** block_levels(key_of[17], (MODEL_DIM,), ((0, 8),), -0.2, 0.2)), 0.5, 2.0),
    }


EPS = 1e-06
DECAY_FACTOR = 8.0

def row_norm(rows, gain_vec):
    values = rows.astype(jnp.float32)
    inverse = lax.rsqrt(lax.optimization_barrier(jnp.mean(values * values, axis=-1, keepdims=True)) + EPS)
    return (values * inverse * gain_vec).astype(jnp.bfloat16)

def combine_pairs(earlier, later):
    decay_one, value_one = earlier
    decay_two, value_two = later
    return (decay_one * decay_two, decay_two * value_one + value_two)

def grouped_sum(left_rows, weight_low, col_scale, groups):
    seq_rows, inner = left_rows.shape
    left_groups = left_rows.reshape(seq_rows, groups, inner // groups).astype(jnp.float32)
    weight_groups = weight_low.reshape(groups, inner // groups, weight_low.shape[1]).astype(jnp.float32)
    parts = jnp.einsum('lgw,gwd->gld', left_groups, weight_groups) * col_scale
    parts_low = parts.astype(jnp.bfloat16)
    parts_low = lax.optimization_barrier(parts_low)
    return lax.optimization_barrier(jnp.sum(parts_low.astype(jnp.float32), axis=0))

def reference(tokens, mixing_norm_gain, recurrent_input_weight, recurrent_input_scale, convolution_kernel_taps, recurrence_gate_weight_blocks, input_gate_weight_blocks, channel_decay_parameter, token_extra_log_decay, mixing_output_weight, mixing_output_scale, feedforward_norm_gain, feedforward_gate_weight, feedforward_gate_scale, feedforward_up_weight, feedforward_up_scale, feedforward_down_weight, feedforward_down_scale):
    rec_low = recurrent_input_weight.astype(jnp.bfloat16)
    mix_low = mixing_output_weight.astype(jnp.bfloat16)
    gate_low = feedforward_gate_weight.astype(jnp.bfloat16)
    up_low = feedforward_up_weight.astype(jnp.bfloat16)
    down_low = feedforward_down_weight.astype(jnp.bfloat16)
    recur_f32 = recurrence_gate_weight_blocks.astype(jnp.float32)
    input_f32 = input_gate_weight_blocks.astype(jnp.float32)

    def single_sequence(packed_arrays):
        sequence_token_rows, sequence_extra_decay = packed_arrays
        normed = row_norm(sequence_token_rows, mixing_norm_gain)
        rec_input = (jnp.dot(normed, rec_low, preferred_element_type=jnp.float32) * recurrent_input_scale).astype(jnp.bfloat16)
        rec_f32 = rec_input.astype(jnp.float32)
        padded = jnp.pad(rec_f32, ((CONV - 1, 0), (0, 0)))
        conv_out = jnp.zeros((SEQUENCE_LENGTH, W), jnp.float32)
        for tap_index in range(CONV):
            conv_out = conv_out + convolution_kernel_taps[tap_index] * padded[tap_index:tap_index + SEQUENCE_LENGTH]
        blocks = conv_out.astype(jnp.bfloat16).reshape(SEQUENCE_LENGTH, NB, BLOCK).astype(jnp.float32)
        recurrence_gate_values = jax.nn.sigmoid(jnp.einsum('lni,nij->lnj', blocks, recur_f32).reshape(SEQUENCE_LENGTH, W))
        input_gate = jax.nn.sigmoid(jnp.einsum('lni,nij->lnj', blocks, input_f32).reshape(SEQUENCE_LENGTH, W))
        decay_logarithm = -DECAY_FACTOR * recurrence_gate_values * jax.nn.softplus(-channel_decay_parameter) + sequence_extra_decay[:, None]
        decay = jnp.exp(decay_logarithm)
        drive = jnp.sqrt(-jnp.expm1(2.0 * decay_logarithm)) * input_gate * conv_out
        _, state = lax.associative_scan(combine_pairs, (decay, drive), axis=0)
        state_low = state.astype(jnp.bfloat16)
        mix_sum = grouped_sum(state_low, mix_low, mixing_output_scale, N_TP)
        mixed = (sequence_token_rows.astype(jnp.float32) + mix_sum).astype(jnp.bfloat16)
        normed_ffn = row_norm(mixed, feedforward_norm_gain)
        ffn_gate = jnp.dot(normed_ffn, gate_low, preferred_element_type=jnp.float32) * feedforward_gate_scale
        ffn_up = jnp.dot(normed_ffn, up_low, preferred_element_type=jnp.float32) * feedforward_up_scale
        hidden = (jax.nn.silu(ffn_gate) * ffn_up).astype(jnp.bfloat16)
        down_sum = grouped_sum(hidden, down_low, feedforward_down_scale, N_TP)
        return (mixed.astype(jnp.float32) + down_sum).astype(jnp.bfloat16)
    sequence_count = TOKENS // SEQUENCE_LENGTH
    output_list = lax.map(single_sequence, (tokens.reshape(sequence_count, SEQUENCE_LENGTH, MODEL_DIM), token_extra_log_decay.reshape(sequence_count, SEQUENCE_LENGTH)))
    return output_list.reshape(TOKENS, MODEL_DIM)
```

```python
import jax
import jax.numpy as jnp
from jax import lax
from jax.experimental import pallas as pl
from jax.experimental.pallas import tpu as pltpu
from jax.sharding import PartitionSpec as P

EPS = 1e-06
DECAY_FACTOR = 8.0


def row_norm(rows, gain_vec):
    values = rows.astype(jnp.float32)
    inverse = lax.rsqrt(jnp.mean(values * values, axis=-1, keepdims=True) + EPS)
    return (values * inverse * gain_vec).astype(jnp.bfloat16)


def gather_normed(rows, gain_vec):
    whole_rows = lax.all_gather(rows, "tp", axis=1, tiled=True)
    return row_norm(whole_rows, gain_vec)


def share_sums(terms):
    return lax.psum_scatter(
        terms.astype(jnp.bfloat16), "tp", scatter_dimension=1, tiled=True
    ).astype(jnp.float32)


def combine_pairs(earlier, later):
    decay_one, value_one = earlier
    decay_two, value_two = later
    return (decay_one * decay_two, decay_two * value_one + value_two)


def add_one(left_rows, weight_piece):
    return jnp.dot(left_rows, weight_piece, preferred_element_type=jnp.float32)


def place_columns(left_rows, total_now, pieces, start_row):
    weight_piece, scale_piece = pieces
    product = jnp.dot(left_rows, weight_piece, preferred_element_type=jnp.float32) * scale_piece
    return lax.dynamic_update_slice_in_dim(total_now, product, start_row, 1)


def plain_body(
    tokens,
    mixing_norm_gain,
    recurrent_input_weight,
    recurrent_input_scale,
    convolution_kernel_taps,
    recurrence_gate_weight_blocks,
    input_gate_weight_blocks,
    channel_decay_parameter,
    token_extra_log_decay,
    mixing_output_weight,
    mixing_output_scale,
    feedforward_norm_gain,
    feedforward_gate_weight,
    feedforward_gate_scale,
    feedforward_up_weight,
    feedforward_up_scale,
    feedforward_down_weight,
    feedforward_down_scale,
):
    normed = gather_normed(tokens, mixing_norm_gain)
    seq_rows = normed.shape[0]
    model_width = normed.shape[1]
    width_dev = recurrent_input_weight.shape[1]
    rec_sum = add_one(
        normed,
        lax.all_gather(recurrent_input_weight.astype(jnp.bfloat16), "fs", axis=0, tiled=True),
    )
    rec_input = (rec_sum * recurrent_input_scale).astype(jnp.bfloat16)
    rec_f32 = rec_input.astype(jnp.float32)
    tap_count = convolution_kernel_taps.shape[0]
    padded = jnp.pad(rec_f32, ((tap_count - 1, 0), (0, 0)))
    conv_out = jnp.zeros((seq_rows, width_dev), jnp.float32)
    for tap_index in range(tap_count):
        conv_out = (
            conv_out + convolution_kernel_taps[tap_index] * padded[tap_index : tap_index + seq_rows]
        )
    block_count = recurrence_gate_weight_blocks.shape[0]
    block_size = recurrence_gate_weight_blocks.shape[1]
    blocks = conv_out.astype(jnp.bfloat16).reshape(seq_rows, block_count, block_size)
    recurrence_gate_values = jax.nn.sigmoid(
        jnp.einsum(
            "lni,nij->lnj",
            blocks,
            recurrence_gate_weight_blocks,
            preferred_element_type=jnp.float32,
        ).reshape(seq_rows, width_dev)
    )
    input_gate = jax.nn.sigmoid(
        jnp.einsum(
            "lni,nij->lnj", blocks, input_gate_weight_blocks, preferred_element_type=jnp.float32
        ).reshape(seq_rows, width_dev)
    )
    decay_logarithm = (
        -DECAY_FACTOR * recurrence_gate_values * jax.nn.softplus(-channel_decay_parameter)
        + token_extra_log_decay[:, None]
    )
    decay = jnp.exp(decay_logarithm)
    drive = jnp.sqrt(-jnp.expm1(2.0 * decay_logarithm)) * input_gate * conv_out
    _, state = lax.associative_scan(combine_pairs, (decay, drive), axis=0)
    state_low = state.astype(jnp.bfloat16)
    mix_terms = place_columns(
        state_low,
        jnp.zeros((seq_rows, model_width), jnp.float32),
        (
            lax.all_gather(mixing_output_weight.astype(jnp.bfloat16), "fs", axis=1, tiled=True),
            lax.all_gather(
                mixing_output_scale.reshape(1, -1).astype(jnp.bfloat16), "fs", axis=1, tiled=True
            ).astype(jnp.float32),
        ),
        jnp.int32(0),
    )
    mixed = (tokens.astype(jnp.float32) + share_sums(mix_terms)).astype(jnp.bfloat16)
    normed_ffn = gather_normed(mixed, feedforward_norm_gain)
    gate_sum = add_one(
        normed_ffn,
        lax.all_gather(feedforward_gate_weight.astype(jnp.bfloat16), "fs", axis=0, tiled=True),
    )
    up_sum = add_one(
        normed_ffn,
        lax.all_gather(feedforward_up_weight.astype(jnp.bfloat16), "fs", axis=0, tiled=True),
    )
    hidden = (
        jax.nn.silu(gate_sum * feedforward_gate_scale) * (up_sum * feedforward_up_scale)
    ).astype(jnp.bfloat16)
    down_terms = place_columns(
        hidden,
        jnp.zeros((seq_rows, model_width), jnp.float32),
        (
            lax.all_gather(feedforward_down_weight.astype(jnp.bfloat16), "fs", axis=1, tiled=True),
            lax.all_gather(
                feedforward_down_scale.reshape(1, -1).astype(jnp.bfloat16), "fs", axis=1, tiled=True
            ).astype(jnp.float32),
        ),
        jnp.int32(0),
    )
    return (mixed.astype(jnp.float32) + share_sums(down_terms)).astype(jnp.bfloat16)


def rec_kernel(rec_ref, taps_ref, wr_ref, wi_ref, decay_ref, extra_ref, out_ref):
    values = rec_ref[0].astype(jnp.float32)
    rows = lax.broadcasted_iota(jnp.int32, values.shape, 0)
    tap_count = taps_ref.shape[0]
    conv_out = taps_ref[tap_count - 1][None, :] * values
    for back in range(1, tap_count):
        moved = jnp.where(rows >= back, pltpu.roll(values, back, 0), 0.0)
        conv_out = conv_out + taps_ref[tap_count - 1 - back][None, :] * moved
    low = conv_out.astype(jnp.bfloat16)
    recur = jax.nn.sigmoid(jnp.dot(low, wr_ref[0], preferred_element_type=jnp.float32))
    inp = jax.nn.sigmoid(jnp.dot(low, wi_ref[0], preferred_element_type=jnp.float32))
    param = -decay_ref[0]
    soft = jnp.maximum(param, 0.0) + jnp.log1p(jnp.exp(-jnp.abs(param)))
    log_decay = -DECAY_FACTOR * recur * soft[None, :] + extra_ref[0]
    decay = jnp.exp(log_decay)
    drive = jnp.sqrt(-jnp.tanh(log_decay) * (1.0 + decay * decay)) * inp * conv_out
    step = 1
    while step < values.shape[0]:
        keep = rows >= step
        drive = drive + decay * jnp.where(keep, pltpu.roll(drive, step, 0), 0.0)
        if step * 2 < values.shape[0]:
            decay = decay * jnp.where(keep, pltpu.roll(decay, step, 0), 1.0)
        step *= 2
    out_ref[0] = drive.astype(jnp.bfloat16)


def recurrence(rec_input, taps, wr, wi, decay_param, extra):
    seqs, rows, chans = rec_input.shape
    blocks, size = wr.shape[0], wr.shape[1]
    return pl.pallas_call(
        rec_kernel,
        grid=(seqs, blocks),
        in_specs=[
            pl.BlockSpec((1, rows, size), lambda s, b: (s, 0, b)),
            pl.BlockSpec((taps.shape[0], size), lambda s, b: (0, b)),
            pl.BlockSpec((1, size, size), lambda s, b: (b, 0, 0)),
            pl.BlockSpec((1, size, size), lambda s, b: (b, 0, 0)),
            pl.BlockSpec((1, size), lambda s, b: (0, b)),
            pl.BlockSpec((1, rows, 1), lambda s, b: (s, 0, 0)),
        ],
        out_specs=pl.BlockSpec((1, rows, size), lambda s, b: (s, 0, b)),
        out_shape=jax.ShapeDtypeStruct(rec_input.shape, jnp.bfloat16),
        cost_estimate=pl.CostEstimate(
            flops=rec_input.size * 600, bytes_accessed=rec_input.size * 4, transcendentals=rec_input.size * 6
        ),
    )(rec_input, taps, wr, wi, decay_param.reshape(1, -1), extra[..., None])


def swap(value, axis, stride=1):
    count = lax.axis_size(axis)
    return lax.ppermute(value, axis, [(i, i ^ 1) for i in range(count)])


def team_gather(rows):
    half = rows.shape[0] // 2
    first, second = rows[:half], rows[half:]
    first = jnp.stack([first, swap(first, "rep")], 0)
    second = jnp.stack([second, swap(second, "fs")], 0)
    first = jnp.stack([first, swap(first, "fs")], 1)
    second = jnp.stack([second, swap(second, "rep")], 0)
    mine = jnp.concatenate([first, second], 2)
    mine = mine.reshape((4,) + mine.shape[2:])
    other = swap(mine, "tp")
    t = lax.axis_index("tp")
    return jnp.concatenate(
        [jnp.where(t == 0, mine, other), jnp.where(t == 0, other, mine)], -1
    )


def take_half(value, axis, which):
    size = value.shape[axis] // 2
    return lax.dynamic_slice_in_dim(value, which * size, size, axis)


def add_low(one, two):
    return (one.astype(jnp.float32) + two.astype(jnp.float32)).astype(jnp.bfloat16)


def team_sum(part):
    t = lax.axis_index("tp")
    kept = add_low(take_half(part, 1, t), swap(take_half(part, 1, 1 - t), "tp"))
    kept = kept.reshape((2, 2) + kept.shape[1:])
    half = kept.shape[2] // 2
    first, second = kept[:, :, :half], kept[:, :, half:]
    first = add_low(first[0], swap(first[1], "rep"))
    second = add_low(second[:, 0], swap(second[:, 1], "fs"))
    first = first[0].astype(jnp.float32) + swap(first[1], "fs").astype(jnp.float32)
    second = second[0].astype(jnp.float32) + swap(second[1], "rep").astype(jnp.float32)
    return jnp.concatenate([first, second], 0)


def to_features(rows_f32):
    low = rows_f32.astype(jnp.bfloat16)
    t = lax.axis_index("tp")
    mine = take_half(low, 1, t)
    other = swap(take_half(low, 1, 1 - t), "tp")
    return jnp.concatenate(
        [jnp.where(t == 0, mine, other), jnp.where(t == 0, other, mine)], 0
    )


def quarter(value, axis, rep, pair):
    size = value.shape[axis] // 4
    return lax.dynamic_slice_in_dim(value, (rep * 2 + pair) * size, size, axis)


def pair_blocks(weight, cut_axis, join_axis):
    r, y = lax.axis_index("rep"), lax.axis_index("fs") % 2
    mine = quarter(weight, cut_axis, r, y)
    other = swap(quarter(weight, cut_axis, r, 1 - y), "fs")
    return jnp.concatenate(
        [jnp.where(y == 0, mine, other), jnp.where(y == 0, other, mine)], join_axis
    )


def line_blocks(block):
    count = lax.axis_size("fs")
    places = count // 2
    z = lax.axis_index("fs") // 2
    up = [(i, i + 2) for i in range(count - 2)]
    down = [(i + 2, i) for i in range(count - 2)]
    from_low, from_high = [block], [block]
    for _ in range(places - 1):
        from_low.append(lax.ppermute(from_low[-1], "fs", up))
        from_high.append(lax.ppermute(from_high[-1], "fs", down))
    blocks = [block]
    for d in range(1, places):
        blocks.append(jnp.where(z + d < places, from_high[d], from_low[places - d]))
    return blocks


def row_product(left, blocks):
    z = lax.axis_index("fs") // 2
    depth = blocks[0].shape[0]
    total = 0.0
    for d, block in enumerate(blocks):
        piece = lax.dynamic_slice_in_dim(left, ((z + d) % len(blocks)) * depth, depth, left.ndim - 1)
        total = total + jnp.dot(piece, block, preferred_element_type=jnp.float32)
    return total


def column_sums(left, blocks):
    z = lax.axis_index("fs") // 2
    width = blocks[0].shape[1]
    sums = None
    for d, block in enumerate(blocks):
        part = jnp.dot(left, block, preferred_element_type=jnp.float32).astype(jnp.bfloat16)
        piece = team_sum(part)
        if sums is None:
            sums = jnp.zeros((piece.shape[0], width * len(blocks)), jnp.float32)
        sums = lax.dynamic_update_slice_in_dim(sums, piece, ((z + d) % len(blocks)) * width, 1)
    return to_features(sums)


def team_body(
    tokens,
    mixing_norm_gain,
    recurrent_input_weight,
    recurrent_input_scale,
    convolution_kernel_taps,
    recurrence_gate_weight_blocks,
    input_gate_weight_blocks,
    channel_decay_parameter,
    token_extra_log_decay,
    mixing_output_weight,
    mixing_output_scale,
    feedforward_norm_gain,
    feedforward_gate_weight,
    feedforward_gate_scale,
    feedforward_up_weight,
    feedforward_up_scale,
    feedforward_down_weight,
    feedforward_down_scale,
):
    r, y = lax.axis_index("rep"), lax.axis_index("fs") % 2
    low = jnp.bfloat16
    rec_blocks = line_blocks(pair_blocks(recurrent_input_weight.astype(low), 1, 0))
    gathered = team_gather(tokens)
    mix_blocks = line_blocks(pair_blocks((mixing_output_weight * mixing_output_scale).astype(low), 0, 1))
    gate_blocks = line_blocks(pair_blocks(feedforward_gate_weight.astype(low), 1, 0))
    up_blocks = line_blocks(pair_blocks(feedforward_up_weight.astype(low), 1, 0))
    down_blocks = line_blocks(
        pair_blocks((feedforward_down_weight * feedforward_down_scale).astype(low), 0, 1)
    )
    extra = jnp.stack([token_extra_log_decay, swap(token_extra_log_decay, "rep")], 0)
    extra = jnp.stack([extra, swap(extra, "fs")], 1).reshape(4, -1)

    normed = row_norm(gathered, mixing_norm_gain)
    rec_input = (
        row_product(normed, rec_blocks) * quarter(recurrent_input_scale, 0, r, y)
    ).astype(low)
    state_low = recurrence(
        rec_input,
        quarter(convolution_kernel_taps, 1, r, y),
        quarter(recurrence_gate_weight_blocks, 0, r, y),
        quarter(input_gate_weight_blocks, 0, r, y),
        quarter(channel_decay_parameter, 0, r, y),
        extra,
    )
    mix_sum = column_sums(state_low, mix_blocks)
    mixed = (tokens.astype(jnp.float32) + mix_sum.astype(jnp.float32)).astype(low)
    normed_ffn = row_norm(team_gather(mixed), feedforward_norm_gain)
    gate = row_product(normed_ffn, gate_blocks) * quarter(feedforward_gate_scale, 0, r, y)
    up = row_product(normed_ffn, up_blocks) * quarter(feedforward_up_scale, 0, r, y)
    hidden = (jax.nn.silu(gate) * up).astype(low)
    down_sum = column_sums(hidden, down_blocks)
    return (mixed.astype(jnp.float32) + down_sum.astype(jnp.float32)).astype(low)


def body(*args):
    fits = (
        lax.axis_size("rep") == 2
        and lax.axis_size("tp") == 2
        and lax.axis_size("fs") % 2 == 0
        and args[5].shape[0] % 4 == 0
        and args[12].shape[1] % 512 == 0
    )
    return team_body(*args) if fits else plain_body(*args)


def solution(mesh):
    placed = (
        P(("rep", "fs"), "tp"),
        P(),
        P("fs", "tp"),
        P("tp"),
        P(None, "tp"),
        P("tp", None, None),
        P("tp", None, None),
        P("tp"),
        P(("rep", "fs")),
        P("tp", "fs"),
        P("fs"),
        P(),
        P("fs", "tp"),
        P("tp"),
        P("fs", "tp"),
        P("tp"),
        P("tp", "fs"),
        P("fs"),
    )
    return jax.shard_map(
        body, mesh=mesh, in_specs=placed, out_specs=P(("rep", "fs"), "tp"), check_vma=False
    )
```
